32 devices in a mesh: rep: 8 (over z, y), fs: 2 (over x), tp: 2 (over core).
Axes of the slice: x: 2, y: 2, z: 4, core: 2. Of those that a mesh axis runs over, the one named last changes fastest.
Arguments:
- tokens: bfloat16 [8192, 1024], P(('rep', 'fs', 'tp')), may hold values from -6 to 6
- cotangent: bfloat16 [8192, 1024], P(('rep', 'fs', 'tp')), may hold values from -8 to 8
- gate_weight: bfloat16 [1024, 2816], P(None, ('fs', 'tp')), may hold values from -0.1875 to 0.1875
- value_weight: bfloat16 [1024, 2816], P(None, ('fs', 'tp')), may hold values from -0.1875 to 0.1875
- down_weight: bfloat16 [2816, 1024], P(('fs', 'tp')), may hold values from -0.109375 to 0.109375
- gate_taps: float32 [3, 2816], P(None, ('fs', 'tp')), may hold values from -3.5 to 3.5
- value_taps: float32 [3, 2816], P(None, ('fs', 'tp')), may hold values from -3.5 to 3.5
Outputs:
- input_grad: bfloat16 [8192, 1024], P(('rep', 'fs', 'tp'))
- gate_grad: float32 [1024, 2816], P(None, ('fs', 'tp'))
- value_grad: float32 [1024, 2816], P(None, ('fs', 'tp'))
- down_grad: float32 [2816, 1024], P(('fs', 'tp'))
- gate_taps_grad: float32 [3, 2816], P(None, ('fs', 'tp'))
- value_taps_grad: float32 [3, 2816], P(None, ('fs', 'tp'))
The draws below stay inside these ranges and needn't reach their ends.
All inputs are finite; a program needn't handle non-finite values.
Results may differ from the reference program's by a relative error of at most 0.0062.
Values may be sent and summed in bfloat16 or wider, within the bound.
A program may use at most 128 MiB of HBM per device.

```python
import jax
import jax.numpy as jnp
from jax import lax

D = 1024
FF = 2816
TAPS = 3
SEQ = 1024
TOKENS = 8192
N_REP = 8


def strengthened(entries, own_key, source, target, blocks, factor):
    def block_of(dim):
        return (jnp.arange(entries.shape[dim]) // (entries.shape[dim] // blocks)).reshape((-1,) + (1,) * (entries.ndim - 1 - dim))

    first = jax.random.permutation(own_key, blocks)[block_of(target)]
    other_side = (block_of(target) + blocks // 2) % blocks
    return jnp.where((block_of(source) == first) | (block_of(source) == other_side), factor * entries, entries)


def steps_of(stream_key, shape, cuts, least, high):
    level = 1.0
    for axis_at, blocks in cuts:
        draws = jax.random.uniform(jax.random.fold_in(jax.random.fold_in(stream_key, 6), axis_at), (blocks,), jnp.float32, least / len(cuts), high / len(cuts))
        level = level * jnp.repeat(jnp.exp(draws), shape[axis_at] // blocks).reshape((-1,) + (1,) * (len(shape) - 1 - axis_at))
    return level


def centred(stream_key, dims, deviation, reach, cuts=(), dtype=jnp.bfloat16):
    entries = deviation * jax.random.normal(stream_key, dims, jnp.float32)
    if cuts:
        entries = entries * steps_of(stream_key, dims, cuts, -0.22, 0.18)
    return jnp.clip(entries, -reach, reach).astype(dtype)


def heavy_noise(own_key, dims, width, limit, pieces, heavy, held_as=jnp.bfloat16):
    entries = width * jax.random.normal(own_key, dims, jnp.float32)
    if pieces:
        entries = entries * steps_of(own_key, dims, pieces, -0.22, 0.18)
    return jnp.clip(strengthened(entries, jax.random.fold_in(own_key, 3), *heavy), -limit, limit).astype(held_as)


def setup_inputs(seed: int = 0) -> dict:
    keys = jax.random.split(jax.random.key(seed), 8)
    tokens = centred(keys[0], (TOKENS, D), 1.0, 6.0, ((0, 32),))
    cotangent = heavy_noise(keys[1], (TOKENS, D), 1.0, 8.0, ((0, 32),), (0, 1, 32, 2.75))
    gate_weight = centred(keys[2], (D, FF), D ** -0.5, 0.1875, ((1, 4),))
    value_weight = centred(keys[3], (D, FF), D ** -0.5, 0.1875, ((1, 4),))
    down_weight = centred(keys[4], (FF, D), FF ** -0.5, 0.109375, ((0, 4),))
    gate_taps = centred(keys[5], (TAPS, FF), TAPS ** -0.5, 3.5, ((1, 4),), jnp.float32)
    value_taps = centred(keys[6], (TAPS, FF), TAPS ** -0.5, 3.5, ((1, 4),), jnp.float32)
    return {"tokens": tokens, "cotangent": cotangent, "gate_weight": gate_weight, "value_weight": value_weight, "down_weight": down_weight, "gate_taps": gate_taps, "value_taps": value_taps}


def shift_back(field, offset):
    return jnp.pad(field, ((offset, 0), (0, 0)))[:field.shape[0]]


def shift_ahead(field, offset):
    return jnp.pad(field, ((0, offset), (0, 0)))[offset:]


def causal_mix(field, taps):
    total = taps[0][None, :] * field
    for offset in range(1, TAPS):
        total = total + taps[offset][None, :] * shift_back(field, offset)
    return total


def reverse_mix(field, taps):
    total = taps[0][None, :] * field
    for offset in range(1, TAPS):
        total = total + taps[offset][None, :] * shift_ahead(field, offset)
    return total


def tap_sums(back, field):
    return jnp.stack([jnp.sum(back * shift_back(field, offset), axis=0) for offset in range(TAPS)])


def contract_rows(left, right):
    return lax.dot_general(left, right, (((0,), (0,)), ((), ())), preferred_element_type=jnp.float32)


def contract_cols(left, right):
    return lax.dot_general(left, right, (((1,), (1,)), ((), ())), preferred_element_type=jnp.float32)


def reference(tokens, cotangent, gate_weight, value_weight, down_weight, gate_taps, value_taps):
    rows_all = tokens.reshape(N_REP, SEQ, D)
    cots_all = cotangent.reshape(N_REP, SEQ, D)

    def one_sequence(carry, pair):
        rows, cots = pair
        up_gate = lax.optimization_barrier(jnp.dot(rows, gate_weight, preferred_element_type=jnp.float32).astype(jnp.bfloat16)).astype(jnp.float32)
        up_value = lax.optimization_barrier(jnp.dot(rows, value_weight, preferred_element_type=jnp.float32).astype(jnp.bfloat16)).astype(jnp.float32)
        conv_gate = causal_mix(up_gate, gate_taps)
        conv_value = causal_mix(up_value, value_taps)
        sigma = jax.nn.sigmoid(conv_gate)
        silu_gate = conv_gate * sigma
        hidden = (silu_gate * conv_value).astype(jnp.bfloat16)
        back_hidden = contract_cols(cots, down_weight)
        back_value = back_hidden * silu_gate
        back_gate = back_hidden * conv_value * sigma * (1.0 + conv_gate * (1.0 - sigma))
        grad_gate = reverse_mix(back_gate, gate_taps).astype(jnp.bfloat16)
        grad_value = reverse_mix(back_value, value_taps).astype(jnp.bfloat16)
        input_grad = (contract_cols(grad_gate, gate_weight) + contract_cols(grad_value, value_weight)).astype(jnp.bfloat16)
        new_carry = (carry[0] + contract_rows(rows, grad_gate),
                     carry[1] + contract_rows(rows, grad_value),
                     carry[2] + contract_rows(hidden, cots),
                     carry[3] + tap_sums(back_gate, up_gate),
                     carry[4] + tap_sums(back_value, up_value))
        return new_carry, input_grad

    start = (jnp.zeros((D, FF), jnp.float32), jnp.zeros((D, FF), jnp.float32),
             jnp.zeros((FF, D), jnp.float32), jnp.zeros((TAPS, FF), jnp.float32),
             jnp.zeros((TAPS, FF), jnp.float32))
    sums, grads = lax.scan(one_sequence, start, (rows_all, cots_all))
    scale = TOKENS ** -0.5
    return (grads.reshape(TOKENS, D), sums[0] * scale, sums[1] * scale, sums[2] * scale,
            sums[3] * scale, sums[4] * scale)
```

```python
import functools
import math

import jax
import jax.numpy as jnp
from jax import lax
from jax.experimental import pallas as pl
from jax.experimental.pallas import tpu as pltpu
from jax.sharding import PartitionSpec as P


def shift_back(field, offset):
    return jnp.pad(field, ((offset, 0), (0, 0)))[: field.shape[0]]


def shift_ahead(field, offset):
    return jnp.pad(field, ((0, offset), (0, 0)))[offset:]


def causal_mix(field, taps):
    total = taps[0][None, :] * field
    for offset in range(1, taps.shape[0]):
        total = total + taps[offset][None, :] * shift_back(field, offset)
    return total


def reverse_mix(field, taps):
    total = taps[0][None, :] * field
    for offset in range(1, taps.shape[0]):
        total = total + taps[offset][None, :] * shift_ahead(field, offset)
    return total


def tap_sums(back, field, count):
    return jnp.stack([jnp.sum(back * shift_back(field, offset), axis=0) for offset in range(count)])


def contract_rows(left, right):
    return lax.dot_general(
        left, right, (((0,), (0,)), ((), ())), preferred_element_type=jnp.float32
    )


def contract_cols(left, right):
    return lax.dot_general(
        left, right, (((1,), (1,)), ((), ())), preferred_element_type=jnp.float32
    )

MESH = pl.DeviceIdType.MESH


def send(src, dst, send_sem, recv_sem, where):
    return pltpu.make_async_remote_copy(
        src_ref=src, dst_ref=dst, send_sem=send_sem, recv_sem=recv_sem, device_id=where, device_id_type=MESH
    )


def reduce_kernel(
    n, fs, tp, scale,
    gv, dn, ig, taps,
    gv_out, dn_out, ig_out, taps_out,
    gv_y, dn_y, gv_z, dn_z, gv_in, dn_in, ig_in, taps_in,
    y_send, y_recv, z_send, z_recv, az_send, az_recv, ay_send, ay_recv, ig_send, ig_recv, t_send, t_recv,
):
    depth = n // 2
    me = lax.axis_index("rep")
    y, z = lax.rem(me, 2), lax.div(me, 2)
    partner = me + 1 - 2 * y
    my_fs, my_tp = lax.axis_index("fs"), lax.axis_index("tp")
    rows = gv.shape[0] // n
    cols = dn.shape[1] // n
    group = fs * tp
    ig_rows = ig.shape[0] // group
    mine = my_fs * tp + my_tp

    def gv_rows(chunk):
        return pl.ds(pl.multiple_of(chunk * rows, rows), rows)

    def dn_cols(chunk):
        return pl.ds(pl.multiple_of(chunk * cols, cols), cols)

    def mate(offset):
        spot = lax.rem(mine + offset, group)
        return spot, {"fs": lax.div(spot, tp), "tp": lax.rem(spot, tp)}

    barrier = pltpu.get_barrier_semaphore()
    for offset in range(1, n):
        pl.semaphore_signal(barrier, inc=1, device_id={"rep": lax.rem(me + offset, n)}, device_id_type=MESH)
    for offset in range(1, group):
        pl.semaphore_signal(barrier, inc=1, device_id=mate(offset)[1], device_id_type=MESH)
    pl.semaphore_wait(barrier, n - 1 + group - 1)

    order = list(range(1, depth)) + [0]
    first = []
    for k in order:
        zt = lax.rem(z + k, depth)
        theirs = 2 * zt + 1 - y
        pair = (
            send(gv.at[gv_rows(theirs), :], gv_y.at[k], y_send.at[0, k], y_recv.at[0, k], {"rep": partner}),
            send(dn.at[:, dn_cols(theirs)], dn_y.at[k], y_send.at[1, k], y_recv.at[1, k], {"rep": partner}),
        )
        for c in pair:
            c.start()
        first.append(pair)
    igs = []
    for offset in range(1, group):
        spot, where = mate(offset)
        c = send(
            ig.at[pl.ds(pl.multiple_of(spot * ig_rows, ig_rows), ig_rows), :], ig_in.at[offset - 1],
            ig_send.at[offset - 1], ig_recv.at[offset - 1], where,
        )
        c.start()
        igs.append(c)
    tcs = []
    for offset in range(1, n):
        c = send(taps, taps_in.at[me], t_send.at[offset - 1], t_recv.at[offset - 1], {"rep": lax.rem(me + offset, n)})
        c.start()
        tcs.append(c)

    second = []
    for i, k in enumerate(order):
        zt = lax.rem(z + k, depth)
        ours = 2 * zt + y
        first[i][0].wait_recv()
        gv_z[k] = (gv[gv_rows(ours), :].astype(jnp.float32) + gv_y[k].astype(jnp.float32)).astype(jnp.bfloat16)
        first[i][1].wait_recv()
        dn_z[k] = (dn[:, dn_cols(ours)].astype(jnp.float32) + dn_y[k].astype(jnp.float32)).astype(jnp.bfloat16)
        if k:
            where = {"rep": ours}
            pair = (
                send(gv_z.at[k], gv_in.at[k], z_send.at[0, k], z_recv.at[0, k], where),
                send(dn_z.at[k], dn_in.at[k], z_send.at[1, k], z_recv.at[1, k], where),
            )
            for c in pair:
                c.start()
            second.append(pair)

    for c in second:
        c[0].wait_recv()
        c[1].wait_recv()
    gv_total = gv_z[0].astype(jnp.float32)
    dn_total = dn_z[0].astype(jnp.float32)
    for k in range(1, depth):
        gv_total = gv_total + gv_in[k].astype(jnp.float32)
        dn_total = dn_total + dn_in[k].astype(jnp.float32)
    gv_out[gv_rows(me), :] = (gv_total * scale).astype(jnp.bfloat16)
    dn_out[:, dn_cols(me)] = (dn_total * scale).astype(jnp.bfloat16)

    def spread(chunk, k, sends, recvs, where):
        pair = (
            send(gv_out.at[gv_rows(chunk), :], gv_out.at[gv_rows(chunk), :], sends.at[0, k], recvs.at[0, k], where),
            send(dn_out.at[:, dn_cols(chunk)], dn_out.at[:, dn_cols(chunk)], sends.at[1, k], recvs.at[1, k], where),
        )
        for c in pair:
            c.start()
        return pair

    third = [spread(me, k, az_send, az_recv, {"rep": 2 * lax.rem(z + k, depth) + y}) for k in range(1, depth)]
    last = [spread(me, 0, ay_send, ay_recv, {"rep": partner})]

    for c in igs:
        c.wait_recv()
    own = ig[pl.ds(pl.multiple_of(mine * ig_rows, ig_rows), ig_rows), :].astype(jnp.float32)
    for slot in range(group - 1):
        own = own + ig_in[slot].astype(jnp.float32)
    ig_out[...] = own.astype(jnp.bfloat16)
    for c in tcs:
        c.wait_recv()
    taps_in[me] = taps[...]
    total = taps_in[0]
    for slot in range(1, n):
        total = total + taps_in[slot]
    taps_out[...] = total * scale

    for k in range(1, depth):
        third[k - 1][0].wait_recv()
        third[k - 1][1].wait_recv()
        last.append(spread(2 * lax.rem(z + depth - k, depth) + y, k, ay_send, ay_recv, {"rep": partner}))
    for pair in last:
        for c in pair:
            c.wait_recv()
    for pair in first + second + third + last:
        for c in pair:
            c.wait_send()
    for c in igs + tcs:
        c.wait_send()


def reduce_all(gv, dn, ig, taps, n, fs, tp, scale):
    depth, group = n // 2, fs * tp
    rows, width = gv.shape[0] // n, gv.shape[1]
    cols, tall = dn.shape[1] // n, dn.shape[0]
    bf16 = jnp.bfloat16
    dma = pltpu.SemaphoreType.DMA
    vmem = pl.BlockSpec(memory_space=pltpu.VMEM)
    gv_slots = pltpu.VMEM((depth, rows, width), bf16)
    dn_slots = pltpu.VMEM((depth, tall, cols), bf16)
    return pl.pallas_call(
        functools.partial(reduce_kernel, n, fs, tp, scale),
        out_shape=(
            jax.ShapeDtypeStruct(gv.shape, bf16),
            jax.ShapeDtypeStruct(dn.shape, bf16),
            jax.ShapeDtypeStruct((ig.shape[0] // group, ig.shape[1]), bf16),
            jax.ShapeDtypeStruct(taps.shape, jnp.float32),
        ),
        in_specs=[vmem] * 4,
        out_specs=(vmem,) * 4,
        scratch_shapes=[
            gv_slots, dn_slots, gv_slots, dn_slots, gv_slots, dn_slots,
            pltpu.VMEM((group - 1, ig.shape[0] // group, ig.shape[1]), bf16),
            pltpu.VMEM((n,) + taps.shape, jnp.float32),
        ] + [dma((2, depth))] * 8 + [dma((group - 1,))] * 2 + [dma((n - 1,))] * 2,
        compiler_params=pltpu.CompilerParams(
            collective_id=0, has_side_effects=True, vmem_limit_bytes=48 * 1024 * 1024
        ),
    )(gv, dn, ig, taps)


def tiles_well(n, fs, tp, gv_rows, gv_cols, dn_rows, dn_cols):
    return (
        n % 2 == 0 and fs * tp > 1 and gv_rows % (16 * n) == 0 and gv_cols % 128 == 0
        and dn_cols % (128 * n) == 0 and dn_rows % 16 == 0 and gv_rows % (16 * fs * tp) == 0
    )


def per_device(tokens, cotangent, gate_weight, value_weight, down_weight, gate_taps, value_taps):
    local_rows = tokens.shape[0]
    hidden_cols = gate_weight.shape[1]
    seq_len = local_rows * lax.axis_size("fs") * lax.axis_size("tp")
    total_tokens = seq_len * lax.axis_size("rep")
    scale = 1.0 / math.sqrt(total_tokens)
    both_weights = jnp.concatenate([gate_weight, value_weight], axis=1)
    piece = lax.all_gather(tokens, ("fs", "tp"), axis=0, tiled=True)
    whole = piece
    block = jnp.dot(piece, both_weights, preferred_element_type=jnp.float32).astype(jnp.bfloat16)
    projected = block
    token_whole, projected = (whole, projected)
    piece = lax.all_gather(cotangent, ("fs", "tp"), axis=0, tiled=True)
    whole = piece
    back = contract_cols(piece, down_weight)
    up_gate = projected[:, :hidden_cols].astype(jnp.float32)
    up_value = projected[:, hidden_cols:].astype(jnp.float32)
    conv_gate = causal_mix(up_gate, gate_taps)
    conv_value = causal_mix(up_value, value_taps)
    sigma = jax.nn.sigmoid(conv_gate)
    silu_gate = conv_gate * sigma
    hidden = (silu_gate * conv_value).astype(jnp.bfloat16)
    back_value = back * silu_gate
    back_gate = back * conv_value * sigma * (1.0 + conv_gate * (1.0 - sigma))
    grad_gate = reverse_mix(back_gate, gate_taps).astype(jnp.bfloat16)
    grad_value = reverse_mix(back_value, value_taps).astype(jnp.bfloat16)
    tap_count = gate_taps.shape[0]
    n, fs, tp = lax.axis_size("rep"), lax.axis_size("fs"), lax.axis_size("tp")
    gate_tap_part = tap_sums(back_gate, up_gate, tap_count)
    value_tap_part = tap_sums(back_value, up_value, tap_count)
    if tiles_well(n, fs, tp, tokens.shape[1], 2 * hidden_cols, hidden_cols, cotangent.shape[1]):
        grads = jnp.concatenate([grad_gate, grad_value], axis=1)
        gv = contract_rows(token_whole, grads).astype(jnp.bfloat16)
        dn = contract_rows(hidden, whole).astype(jnp.bfloat16)
        ig = contract_cols(grads, both_weights).astype(jnp.bfloat16)
        taps = jnp.pad(jnp.concatenate([gate_tap_part, value_tap_part], axis=1), ((0, -tap_count % 8), (0, 0)))
        gv, dn, input_grad, taps = reduce_all(gv, dn, ig, taps, n, fs, tp, scale)
        return (
            input_grad,
            gv[:, :hidden_cols].astype(jnp.float32),
            gv[:, hidden_cols:].astype(jnp.float32),
            dn.astype(jnp.float32),
            taps[:tap_count, :hidden_cols],
            taps[:tap_count, hidden_cols:],
        )
    input_grad = lax.psum_scatter(
        contract_cols(grad_gate, gate_weight) + contract_cols(grad_value, value_weight),
        ("fs", "tp"),
        scatter_dimension=0,
        tiled=True,
    ).astype(jnp.bfloat16)
    gate_part = contract_rows(token_whole, grad_gate)
    value_part = contract_rows(token_whole, grad_value)
    down_part = contract_rows(hidden, whole)
    summed = lax.psum((gate_part, value_part, down_part, gate_tap_part, value_tap_part), "rep")
    weight_out = tuple((item * scale for item in summed))
    return (input_grad, weight_out[0], weight_out[1], weight_out[2], weight_out[3], weight_out[4])


def solution(mesh):
    in_specs = (
        P(("rep", "fs", "tp"), None),
        P(("rep", "fs", "tp"), None),
        P(None, ("fs", "tp")),
        P(None, ("fs", "tp")),
        P(("fs", "tp"), None),
        P(None, ("fs", "tp")),
        P(None, ("fs", "tp")),
    )
    out_specs = (
        P(("rep", "fs", "tp"), None),
        P(None, ("fs", "tp")),
        P(None, ("fs", "tp")),
        P(("fs", "tp"), None),
        P(None, ("fs", "tp")),
        P(None, ("fs", "tp")),
    )
    return jax.shard_map(
        per_device, mesh=mesh, in_specs=in_specs, out_specs=out_specs, check_vma=False
    )
```

```python
import functools
import math

import jax
import jax.numpy as jnp
from jax import lax
from jax.experimental import pallas as pl
from jax.experimental.pallas import tpu as pltpu
from jax.sharding import PartitionSpec as P


def shift_back(field, offset):
    return jnp.pad(field, ((offset, 0), (0, 0)))[: field.shape[0]]


def shift_ahead(field, offset):
    return jnp.pad(field, ((0, offset), (0, 0)))[offset:]


def causal_mix(field, taps):
    total = taps[0][None, :] * field
    for offset in range(1, taps.shape[0]):
        total = total + taps[offset][None, :] * shift_back(field, offset)
    return total


def reverse_mix(field, taps):
    total = taps[0][None, :] * field
    for offset in range(1, taps.shape[0]):
        total = total + taps[offset][None, :] * shift_ahead(field, offset)
    return total


def tap_sums(back, field, count):
    return jnp.stack([jnp.sum(back * shift_back(field, offset), axis=0) for offset in range(count)])


def contract_rows(left, right):
    return lax.dot_general(
        left, right, (((0,), (0,)), ((), ())), preferred_element_type=jnp.float32
    )


def contract_cols(left, right):
    return lax.dot_general(
        left, right, (((1,), (1,)), ((), ())), preferred_element_type=jnp.float32
    )

MESH = pl.DeviceIdType.MESH
BF16 = jnp.bfloat16
F32 = jnp.float32
STRIP = 16
HALO = 8


def send(src, dst, send_sem, recv_sem, where):
    return pltpu.make_async_remote_copy(
        src_ref=src, dst_ref=dst, send_sem=send_sem, recv_sem=recv_sem, device_id=where, device_id_type=MESH
    )


def layer_kernel(
    n, scale,
    tok, cot, gw, vw, dw, gt, vt,
    g_out, v_out, dn_out, ig_out, taps_out,
    tok_all, cot_all, tok_t, hid, hid_t, up_g, up_v, bg, bv, gg, gv,
    g_part, v_part, dn_part, ig_part, taps_acc, taps_mine,
    g_y, v_y, dn_y, g_z, v_z, dn_z, g_in, v_in, dn_in, ig_in, taps_in,
    tok_send, tok_recv, cot_send, cot_recv,
    y_send, y_recv, z_send, z_recv, az_send, az_recv, ay_send, ay_recv, ig_send, ig_recv, t_send, t_recv,
):
    depth = n // 2
    me = lax.axis_index("rep")
    y, z = lax.rem(me, 2), lax.div(me, 2)
    partner = me + 1 - 2 * y
    my_fs, my_tp = lax.axis_index("fs"), lax.axis_index("tp")
    local = tok.shape[0]
    seq = 4 * local
    hidden_cols = gw.shape[1]
    count = gt.shape[0]
    mine = my_fs * 2 + my_tp
    core_spot = my_fs * 2 + 1 - my_tp
    far_spot = (1 - my_fs) * 2 + my_tp
    diag_spot = 3 - mine
    core, far, diag = {"tp": 1 - my_tp}, {"fs": 1 - my_fs}, {"fs": 1 - my_fs, "tp": 1 - my_tp}

    def shard(spot):
        return pl.ds(pl.multiple_of(spot * local, local), local)

    barrier = pltpu.get_barrier_semaphore()
    for offset in range(1, n):
        pl.semaphore_signal(barrier, inc=1, device_id={"rep": lax.rem(me + offset, n)}, device_id_type=MESH)
    for where in (core, far, diag):
        pl.semaphore_signal(barrier, inc=1, device_id=where, device_id_type=MESH)
    pl.semaphore_wait(barrier, n - 1 + 3)

    def gather(own, every, sends, recvs, slot, where):
        c = send(own, every.at[shard(mine), :], sends.at[slot], recvs.at[slot], where)
        c.start()
        return c

    def relay(every, sends, recvs):
        part = every.at[shard(far_spot), :]
        c = send(part, part, sends.at[2], recvs.at[2], core)
        c.start()
        return c

    tok_far = gather(tok, tok_all, tok_send, tok_recv, 0, far)
    tok_core = gather(tok, tok_all, tok_send, tok_recv, 1, core)
    cot_core = gather(cot, cot_all, cot_send, cot_recv, 1, core)
    tok_all[shard(mine), :] = tok[...]
    cot_all[shard(mine), :] = cot[...]
    zeros = jnp.zeros((HALO, hidden_cols), F32)
    up_g[0:HALO, :] = zeros
    up_v[0:HALO, :] = zeros
    bg[seq:seq + HALO, :] = zeros
    bv[seq:seq + HALO, :] = zeros
    taps_acc[...] = jnp.zeros_like(taps_acc)

    def project(spot):
        part = tok_all[shard(spot), :]
        rows = pl.ds(pl.multiple_of(spot * local + HALO, HALO), local)
        up_g[rows, :] = jnp.dot(part, gw[...], preferred_element_type=F32).astype(BF16).astype(F32)
        up_v[rows, :] = jnp.dot(part, vw[...], preferred_element_type=F32).astype(BF16).astype(F32)
        tok_t[:, shard(spot)] = part.T

    project(mine)
    tok_core.wait_recv()
    project(core_spot)
    tok_far.wait_recv()
    cot_far = gather(cot, cot_all, cot_send, cot_recv, 0, far)
    tok_relay = relay(tok_all, tok_send, tok_recv)
    project(far_spot)
    tok_relay.wait_recv()
    project(diag_spot)

    def mix(i, carry):
        start = pl.multiple_of(i * STRIP, STRIP)
        gs = up_g[pl.ds(start, STRIP + HALO), :]
        vs = up_v[pl.ds(start, STRIP + HALO), :]
        conv_gate = gt[0:1, :] * gs[HALO:HALO + STRIP]
        conv_value = vt[0:1, :] * vs[HALO:HALO + STRIP]
        for k in range(1, count):
            conv_gate = conv_gate + gt[k:k + 1, :] * gs[HALO - k:HALO - k + STRIP]
            conv_value = conv_value + vt[k:k + 1, :] * vs[HALO - k:HALO - k + STRIP]
        sigma = jax.nn.sigmoid(conv_gate)
        silu = conv_gate * sigma
        hid[pl.ds(start, STRIP), :] = (silu * conv_value).astype(BF16)
        bv[pl.ds(start, STRIP), :] = silu
        bg[pl.ds(start, STRIP), :] = conv_value * sigma * (1.0 + conv_gate * (1.0 - sigma))
        return carry

    lax.fori_loop(0, seq // STRIP, mix, 0)

    def turn(i, carry):
        rows = pl.ds(pl.multiple_of(i * local, local), local)
        hid_t[:, rows] = hid[rows, :].T
        return carry

    lax.fori_loop(0, 4, turn, 0)

    def pull_back(spot):
        rows = shard(spot)
        back = contract_cols(cot_all[rows, :], dw[...])
        bv[rows, :] = back * bv[rows, :]
        bg[rows, :] = back * bg[rows, :]

    pull_back(mine)
    cot_core.wait_recv()
    pull_back(core_spot)
    cot_far.wait_recv()
    cot_relay = relay(cot_all, cot_send, cot_recv)
    pull_back(far_spot)
    cot_relay.wait_recv()

    g_rows = g_part.shape[0] // n
    d_cols = dn_part.shape[1] // n

    def row_cut(chunk, width=1):
        return (pl.ds(pl.multiple_of(chunk * g_rows, g_rows), g_rows * width), slice(None))

    def col_cut(chunk, width=1):
        return (slice(None), pl.ds(pl.multiple_of(chunk * d_cols, d_cols), d_cols * width))

    order = list(range(1, depth)) + [0]
    kinds = (
        (0, col_cut, dn_part, dn_y, dn_z, dn_in, dn_out),
        (1, row_cut, g_part, g_y, g_z, g_in, g_out),
        (2, row_cut, v_part, v_y, v_z, v_in, v_out),
    )
    waits = []

    def exchange(kind, k):
        index, cut, part, slots = kind[:4]
        theirs = 2 * lax.rem(z + k, depth) + 1 - y
        c = send(part.at[cut(theirs)], slots.at[k], y_send.at[index, k], y_recv.at[index, k], {"rep": partner})
        c.start()
        waits.append(c)
        return c

    def first_stage(kind, product):
        cut, part = kind[1], kind[2]
        sent = {}
        for k in order:
            pair = cut(2 * lax.rem(z + k, depth), 2)
            part[pair] = product(pair).astype(BF16)
            sent[k] = exchange(kind, k)
        return sent

    def second_stage(kind, sent):
        index, cut, part, slots, sums, arrivals = kind[:6]
        passed = []
        for k in order:
            ours = 2 * lax.rem(z + k, depth) + y
            sent[k].wait_recv()
            sums[k] = (part[cut(ours)].astype(F32) + slots[k].astype(F32)).astype(BF16)
            if k:
                c = send(sums.at[k], arrivals.at[k], z_send.at[index, k], z_recv.at[index, k], {"rep": ours})
                c.start()
                waits.append(c)
                passed.append(c)
        return passed

    def spread(kind, chunk, k, sends, recvs, where):
        index, cut, out = kind[0], kind[1], kind[6]
        c = send(out.at[cut(chunk)], out.at[cut(chunk)], sends.at[index, k], recvs.at[index, k], where)
        c.start()
        waits.append(c)
        return c

    def third_stage(kind, passed):
        cut, sums, arrivals, out = kind[1], kind[4], kind[5], kind[6]
        for c in passed:
            c.wait_recv()
        total = sums[0].astype(F32)
        for k in range(1, depth):
            total = total + arrivals[k].astype(F32)
        out[cut(me)] = (total * scale).astype(BF16)
        lines = [spread(kind, me, k, az_send, az_recv, {"rep": 2 * lax.rem(z + k, depth) + y}) for k in range(1, depth)]
        return lines, [spread(kind, me, 0, ay_send, ay_recv, {"rep": partner})]

    def fourth_stage(kind, lines, ends):
        for k in range(1, depth):
            lines[k - 1].wait_recv()
            chunk = 2 * lax.rem(z + depth - k, depth) + y
            ends.append(spread(kind, chunk, k, ay_send, ay_recv, {"rep": partner}))
        return ends

    pull_back(diag_spot)
    dn_sent = first_stage(
        kinds[0], lambda cut: jnp.dot(hid_t[...], cot_all[cut], preferred_element_type=F32)
    )

    def unmix(i, carry):
        start = pl.multiple_of(i * STRIP, STRIP)
        for slot, (field, back, taps, grad) in enumerate(((up_g, bg, gt, gg), (up_v, bv, vt, gv))):
            fs_ = field[pl.ds(start, STRIP + HALO), :]
            bs = back[pl.ds(start, STRIP + HALO), :]
            now = bs[0:STRIP]
            total = taps[0:1, :] * now
            for k in range(1, count):
                total = total + taps[k:k + 1, :] * bs[k:k + STRIP]
            grad[pl.ds(start, STRIP), :] = total.astype(BF16)
            for k in range(count):
                term = now * fs_[HALO - k:HALO - k + STRIP]
                taps_acc[slot * count + k] += term[0:8] + term[8:16]
        return carry

    lax.fori_loop(0, seq // STRIP, unmix, 0)
    g_sent = first_stage(kinds[1], lambda cut: jnp.dot(tok_t[cut], gg[...], preferred_element_type=F32))
    v_sent = first_stage(kinds[2], lambda cut: jnp.dot(tok_t[cut], gv[...], preferred_element_type=F32))

    taps_mine[...] = jnp.sum(taps_acc[...], axis=1)
    taps_sent = []
    for offset in range(1, n):
        c = send(
            taps_mine, taps_in.at[me], t_send.at[offset - 1], t_recv.at[offset - 1],
            {"rep": lax.rem(me + offset, n)},
        )
        c.start()
        taps_sent.append(c)

    dn_passed = second_stage(kinds[0], dn_sent)
    ig_sent = []
    for slot, (spot, where) in enumerate(((far_spot, far), (diag_spot, diag), (core_spot, core), (mine, None))):
        rows = shard(spot)
        ig_part[rows, :] = (contract_cols(gg[rows, :], gw[...]) + contract_cols(gv[rows, :], vw[...])).astype(BF16)
        if where is not None:
            c = send(ig_part.at[rows, :], ig_in.at[slot], ig_send.at[slot], ig_recv.at[slot], where)
            c.start()
            ig_sent.append(c)
    dn_lines, dn_ends = third_stage(kinds[0], dn_passed)
    g_passed = second_stage(kinds[1], g_sent)
    dn_ends = fourth_stage(kinds[0], dn_lines, dn_ends)
    g_lines, g_ends = third_stage(kinds[1], g_passed)
    v_passed = second_stage(kinds[2], v_sent)
    g_ends = fourth_stage(kinds[1], g_lines, g_ends)
    v_lines, v_ends = third_stage(kinds[2], v_passed)

    for c in ig_sent:
        c.wait_recv()
    own = ig_part[shard(mine), :].astype(F32)
    for slot in range(3):
        own = own + ig_in[slot].astype(F32)
    ig_out[...] = own.astype(BF16)
    for c in taps_sent:
        c.wait_recv()
    taps_in[me] = taps_mine[...]
    total = taps_in[0]
    for slot in range(1, n):
        total = total + taps_in[slot]
    taps_out[...] = total * scale

    v_ends = fourth_stage(kinds[2], v_lines, v_ends)
    for c in dn_ends + g_ends + v_ends:
        c.wait_recv()
    for c in waits + taps_sent + ig_sent + [tok_far, tok_core, tok_relay, cot_far, cot_core, cot_relay]:
        c.wait_send()


def whole_layer(tokens, cotangent, gate_weight, value_weight, down_weight, gate_taps, value_taps, n, scale):
    depth = n // 2
    local, model = tokens.shape
    seq = 4 * local
    cols = gate_weight.shape[1]
    count = gate_taps.shape[0]
    dma = pltpu.SemaphoreType.DMA
    vmem = pl.BlockSpec(memory_space=pltpu.VMEM)
    rows_slots = pltpu.VMEM((depth, model // n, cols), BF16)
    cols_slots = pltpu.VMEM((depth, cols, model // n), BF16)
    return pl.pallas_call(
        functools.partial(layer_kernel, n, scale),
        out_shape=(
            jax.ShapeDtypeStruct((model, cols), BF16),
            jax.ShapeDtypeStruct((model, cols), BF16),
            jax.ShapeDtypeStruct((cols, model), BF16),
            jax.ShapeDtypeStruct((local, model), BF16),
            jax.ShapeDtypeStruct((2 * count, cols), F32),
        ),
        in_specs=[vmem] * 7,
        out_specs=(vmem,) * 5,
        scratch_shapes=[
            pltpu.VMEM((seq, model), BF16), pltpu.VMEM((seq, model), BF16), pltpu.VMEM((model, seq), BF16),
            pltpu.VMEM((seq, cols), BF16), pltpu.VMEM((cols, seq), BF16),
            pltpu.VMEM((seq + HALO, cols), F32), pltpu.VMEM((seq + HALO, cols), F32),
            pltpu.VMEM((seq + HALO, cols), F32), pltpu.VMEM((seq + HALO, cols), F32),
            pltpu.VMEM((seq, cols), BF16), pltpu.VMEM((seq, cols), BF16),
            pltpu.VMEM((model, cols), BF16), pltpu.VMEM((model, cols), BF16), pltpu.VMEM((cols, model), BF16),
            pltpu.VMEM((seq, model), BF16),
            pltpu.VMEM((2 * count, 8, cols), F32), pltpu.VMEM((2 * count, cols), F32),
        ] + [rows_slots, rows_slots, cols_slots] * 3 + [
            pltpu.VMEM((3, local, model), BF16), pltpu.VMEM((n, 2 * count, cols), F32),
        ] + [dma((3,))] * 4 + [dma((3, depth))] * 8 + [dma((3,))] * 2 + [dma((n - 1,))] * 2,
        compiler_params=pltpu.CompilerParams(
            collective_id=0, has_side_effects=True, vmem_limit_bytes=60 * 1024 * 1024
        ),
    )(tokens, cotangent, gate_weight, value_weight, down_weight, gate_taps, value_taps)


def tiles_well(n, fs, tp, local, model, cols):
    return (
        n % 2 == 0 and fs == 2 and tp == 2 and model % (128 * n) == 0 and cols % 16 == 0 and local % 128 == 0
        and local * model <= 512 * 1024 and model * cols <= 1024 * 768
    )


def per_device(tokens, cotangent, gate_weight, value_weight, down_weight, gate_taps, value_taps):
    local_rows = tokens.shape[0]
    hidden_cols = gate_weight.shape[1]
    seq_len = local_rows * lax.axis_size("fs") * lax.axis_size("tp")
    total_tokens = seq_len * lax.axis_size("rep")
    scale = 1.0 / math.sqrt(total_tokens)
    n, fs, tp = lax.axis_size("rep"), lax.axis_size("fs"), lax.axis_size("tp")
    if tiles_well(n, fs, tp, local_rows, tokens.shape[1], hidden_cols):
        gate, value, down, input_grad, taps = whole_layer(
            tokens, cotangent, gate_weight, value_weight, down_weight, gate_taps, value_taps, n, scale
        )
        count = gate_taps.shape[0]
        return (
            input_grad, gate.astype(jnp.float32), value.astype(jnp.float32), down.astype(jnp.float32),
            taps[:count], taps[count:],
        )
    both_weights = jnp.concatenate([gate_weight, value_weight], axis=1)
    piece = lax.all_gather(tokens, ("fs", "tp"), axis=0, tiled=True)
    whole = piece
    block = jnp.dot(piece, both_weights, preferred_element_type=jnp.float32).astype(jnp.bfloat16)
    projected = block
    token_whole, projected = (whole, projected)
    piece = lax.all_gather(cotangent, ("fs", "tp"), axis=0, tiled=True)
    whole = piece
    back = contract_cols(piece, down_weight)
    up_gate = projected[:, :hidden_cols].astype(jnp.float32)
    up_value = projected[:, hidden_cols:].astype(jnp.float32)
    conv_gate = causal_mix(up_gate, gate_taps)
    conv_value = causal_mix(up_value, value_taps)
    sigma = jax.nn.sigmoid(conv_gate)
    silu_gate = conv_gate * sigma
    hidden = (silu_gate * conv_value).astype(jnp.bfloat16)
    back_value = back * silu_gate
    back_gate = back * conv_value * sigma * (1.0 + conv_gate * (1.0 - sigma))
    grad_gate = reverse_mix(back_gate, gate_taps).astype(jnp.bfloat16)
    grad_value = reverse_mix(back_value, value_taps).astype(jnp.bfloat16)
    tap_count = gate_taps.shape[0]
    input_grad = lax.psum_scatter(
        contract_cols(grad_gate, gate_weight) + contract_cols(grad_value, value_weight),
        ("fs", "tp"),
        scatter_dimension=0,
        tiled=True,
    ).astype(jnp.bfloat16)
    gate_part = contract_rows(token_whole, grad_gate)
    value_part = contract_rows(token_whole, grad_value)
    down_part = contract_rows(hidden, whole)
    gate_tap_part = tap_sums(back_gate, up_gate, tap_count)
    value_tap_part = tap_sums(back_value, up_value, tap_count)
    summed = lax.psum((gate_part, value_part, down_part, gate_tap_part, value_tap_part), "rep")
    weight_out = tuple((item * scale for item in summed))
    return (input_grad, weight_out[0], weight_out[1], weight_out[2], weight_out[3], weight_out[4])


def solution(mesh):
    in_specs = (
        P(("rep", "fs", "tp"), None),
        P(("rep", "fs", "tp"), None),
        P(None, ("fs", "tp")),
        P(None, ("fs", "tp")),
        P(("fs", "tp"), None),
        P(None, ("fs", "tp")),
        P(None, ("fs", "tp")),
    )
    out_specs = (
        P(("rep", "fs", "tp"), None),
        P(None, ("fs", "tp")),
        P(None, ("fs", "tp")),
        P(("fs", "tp"), None),
        P(None, ("fs", "tp")),
        P(None, ("fs", "tp")),
    )
    return jax.shard_map(
        per_device, mesh=mesh, in_specs=in_specs, out_specs=out_specs, check_vma=False
    )
```

```python
import functools
import math

import jax
import jax.numpy as jnp
from jax import lax
from jax.experimental import pallas as pl
from jax.experimental.pallas import tpu as pltpu
from jax.sharding import PartitionSpec as P


def shift_back(field, offset):
    return jnp.pad(field, ((offset, 0), (0, 0)))[: field.shape[0]]


def shift_ahead(field, offset):
    return jnp.pad(field, ((0, offset), (0, 0)))[offset:]


def causal_mix(field, taps):
    total = taps[0][None, :] * field
    for offset in range(1, taps.shape[0]):
        total = total + taps[offset][None, :] * shift_back(field, offset)
    return total


def reverse_mix(field, taps):
    total = taps[0][None, :] * field
    for offset in range(1, taps.shape[0]):
        total = total + taps[offset][None, :] * shift_ahead(field, offset)
    return total


def tap_sums(back, field, count):
    return jnp.stack([jnp.sum(back * shift_back(field, offset), axis=0) for offset in range(count)])


def contract_rows(left, right):
    return lax.dot_general(
        left, right, (((0,), (0,)), ((), ())), preferred_element_type=jnp.float32
    )


def contract_cols(left, right):
    return lax.dot_general(
        left, right, (((1,), (1,)), ((), ())), preferred_element_type=jnp.float32
    )

MESH = pl.DeviceIdType.MESH
BF16 = jnp.bfloat16
F32 = jnp.float32
STRIP = 16
HALO = 8


def send(src, dst, send_sem, recv_sem, where):
    return pltpu.make_async_remote_copy(
        src_ref=src, dst_ref=dst, send_sem=send_sem, recv_sem=recv_sem, device_id=where, device_id_type=MESH
    )


def layer_kernel(
    n, scale,
    tok, cot, gw, vw, dw, gt, vt,
    g_out, v_out, dn_out, ig_out, taps_out,
    tok_all, cot_all, hid, hid_t, up_g, up_v, bg, bv, gg, gv, gg_t, gv_t,
    g_part, v_part, dn_part, ig_part, taps_acc, taps_mine,
    g_y, v_y, dn_y, g_z, v_z, dn_z, g_in, v_in, dn_in, ig_in, taps_in,
    tok_send, tok_recv, cot_send, cot_recv,
    y_send, y_recv, z_send, z_recv, az_send, az_recv, ay_send, ay_recv, ig_send, ig_recv, t_send, t_recv,
):
    depth = n // 2
    me = lax.axis_index("rep")
    y, z = lax.rem(me, 2), lax.div(me, 2)
    partner = me + 1 - 2 * y
    my_fs, my_tp = lax.axis_index("fs"), lax.axis_index("tp")
    local = tok.shape[0]
    seq = 4 * local
    hidden_cols = gw.shape[0]
    count = gt.shape[0]
    mine = my_fs * 2 + my_tp
    core_spot = my_fs * 2 + 1 - my_tp
    far_spot = (1 - my_fs) * 2 + my_tp
    diag_spot = 3 - mine
    core, far, diag = {"tp": 1 - my_tp}, {"fs": 1 - my_fs}, {"fs": 1 - my_fs, "tp": 1 - my_tp}

    def shard(spot):
        return pl.ds(pl.multiple_of(spot * local, local), local)

    barrier = pltpu.get_barrier_semaphore()
    for offset in range(1, n):
        pl.semaphore_signal(barrier, inc=1, device_id={"rep": lax.rem(me + offset, n)}, device_id_type=MESH)
    for where in (core, far, diag):
        pl.semaphore_signal(barrier, inc=1, device_id=where, device_id_type=MESH)
    pl.semaphore_wait(barrier, n - 1 + 3)

    def gather(own, every, sends, recvs, slot, where):
        c = send(own, every.at[shard(mine), :], sends.at[slot], recvs.at[slot], where)
        c.start()
        return c

    def relay(every, sends, recvs):
        part = every.at[shard(far_spot), :]
        c = send(part, part, sends.at[2], recvs.at[2], core)
        c.start()
        return c

    tok_far = gather(tok, tok_all, tok_send, tok_recv, 0, far)
    tok_core = gather(tok, tok_all, tok_send, tok_recv, 1, core)
    cot_core = gather(cot, cot_all, cot_send, cot_recv, 1, core)
    tok_all[shard(mine), :] = tok[...]
    cot_all[shard(mine), :] = cot[...]
    zeros = jnp.zeros((HALO, hidden_cols), F32)
    up_g[0:HALO, :] = zeros
    up_v[0:HALO, :] = zeros
    bg[seq:seq + HALO, :] = zeros
    bv[seq:seq + HALO, :] = zeros
    taps_acc[...] = jnp.zeros_like(taps_acc)

    def project(spot):
        part = tok_all[shard(spot), :]
        rows = pl.ds(pl.multiple_of(spot * local + HALO, HALO), local)
        up_g[rows, :] = contract_cols(part, gw[...]).astype(BF16).astype(F32)
        up_v[rows, :] = contract_cols(part, vw[...]).astype(BF16).astype(F32)

    project(mine)
    tok_core.wait_recv()
    project(core_spot)
    tok_far.wait_recv()
    cot_far = gather(cot, cot_all, cot_send, cot_recv, 0, far)
    tok_relay = relay(tok_all, tok_send, tok_recv)
    project(far_spot)
    tok_relay.wait_recv()
    project(diag_spot)

    def mix(i, carry):
        start = pl.multiple_of(i * STRIP, STRIP)
        gs = up_g[pl.ds(start, STRIP + HALO), :]
        vs = up_v[pl.ds(start, STRIP + HALO), :]
        conv_gate = gt[0:1, :] * gs[HALO:HALO + STRIP]
        conv_value = vt[0:1, :] * vs[HALO:HALO + STRIP]
        for k in range(1, count):
            conv_gate = conv_gate + gt[k:k + 1, :] * gs[HALO - k:HALO - k + STRIP]
            conv_value = conv_value + vt[k:k + 1, :] * vs[HALO - k:HALO - k + STRIP]
        sigma = jax.nn.sigmoid(conv_gate)
        silu = conv_gate * sigma
        hid[pl.ds(start, STRIP), :] = (silu * conv_value).astype(BF16)
        bv[pl.ds(start, STRIP), :] = silu
        bg[pl.ds(start, STRIP), :] = conv_value * sigma * (1.0 + conv_gate * (1.0 - sigma))
        return carry

    lax.fori_loop(0, seq // STRIP, mix, 0)

    def turn(pairs):
        def step(i, carry):
            rows = pl.ds(pl.multiple_of(i * local, local), local)
            for flat, tall in pairs:
                tall[:, rows] = flat[rows, :].T
            return carry

        lax.fori_loop(0, 4, step, 0)

    turn(((hid, hid_t),))

    def pull_back(spot):
        rows = shard(spot)
        back = contract_cols(cot_all[rows, :], dw[...])
        bv[rows, :] = back * bv[rows, :]
        bg[rows, :] = back * bg[rows, :]

    pull_back(mine)
    cot_core.wait_recv()
    pull_back(core_spot)
    cot_far.wait_recv()
    cot_relay = relay(cot_all, cot_send, cot_recv)
    pull_back(far_spot)
    cot_relay.wait_recv()

    d_cols = dn_part.shape[1] // n

    def col_cut(chunk, width=1):
        return (slice(None), pl.ds(pl.multiple_of(chunk * d_cols, d_cols), d_cols * width))

    order = list(range(1, depth)) + [0]
    kinds = (
        (0, col_cut, dn_part, dn_y, dn_z, dn_in, dn_out),
        (1, col_cut, g_part, g_y, g_z, g_in, g_out),
        (2, col_cut, v_part, v_y, v_z, v_in, v_out),
    )
    waits = []

    def exchange(kind, k):
        index, cut, part, slots = kind[:4]
        theirs = 2 * lax.rem(z + k, depth) + 1 - y
        c = send(part.at[cut(theirs)], slots.at[k], y_send.at[index, k], y_recv.at[index, k], {"rep": partner})
        c.start()
        waits.append(c)
        return c

    def first_stage(kind, product):
        cut, part = kind[1], kind[2]
        sent = {}
        for k in order:
            pair = cut(2 * lax.rem(z + k, depth), 2)
            part[pair] = product(pair).astype(BF16)
            sent[k] = exchange(kind, k)
        return sent

    def second_stage(kind, sent):
        index, cut, part, slots, sums, arrivals = kind[:6]
        passed = []
        for k in order:
            ours = 2 * lax.rem(z + k, depth) + y
            sent[k].wait_recv()
            sums[k] = (part[cut(ours)].astype(F32) + slots[k].astype(F32)).astype(BF16)
            if k:
                c = send(sums.at[k], arrivals.at[k], z_send.at[index, k], z_recv.at[index, k], {"rep": ours})
                c.start()
                waits.append(c)
                passed.append(c)
        return passed

    def spread(kind, chunk, k, sends, recvs, where):
        index, cut, out = kind[0], kind[1], kind[6]
        c = send(out.at[cut(chunk)], out.at[cut(chunk)], sends.at[index, k], recvs.at[index, k], where)
        c.start()
        waits.append(c)
        return c

    def third_stage(kind, passed):
        cut, sums, arrivals, out = kind[1], kind[4], kind[5], kind[6]
        for c in passed:
            c.wait_recv()
        total = sums[0].astype(F32)
        for k in range(1, depth):
            total = total + arrivals[k].astype(F32)
        out[cut(me)] = (total * scale).astype(BF16)
        lines = [spread(kind, me, k, az_send, az_recv, {"rep": 2 * lax.rem(z + k, depth) + y}) for k in range(1, depth)]
        return lines, [spread(kind, me, 0, ay_send, ay_recv, {"rep": partner})]

    def fourth_stage(kind, lines, ends):
        for k in range(1, depth):
            lines[k - 1].wait_recv()
            chunk = 2 * lax.rem(z + depth - k, depth) + y
            ends.append(spread(kind, chunk, k, ay_send, ay_recv, {"rep": partner}))
        return ends

    pull_back(diag_spot)
    dn_sent = first_stage(
        kinds[0], lambda cut: jnp.dot(hid_t[...], cot_all[cut], preferred_element_type=F32)
    )

    def unmix(i, carry):
        start = pl.multiple_of(i * STRIP, STRIP)
        for slot, (field, back, taps, grad) in enumerate(((up_g, bg, gt, gg), (up_v, bv, vt, gv))):
            fs_ = field[pl.ds(start, STRIP + HALO), :]
            bs = back[pl.ds(start, STRIP + HALO), :]
            now = bs[0:STRIP]
            total = taps[0:1, :] * now
            for k in range(1, count):
                total = total + taps[k:k + 1, :] * bs[k:k + STRIP]
            grad[pl.ds(start, STRIP), :] = total.astype(BF16)
            for k in range(count):
                term = now * fs_[HALO - k:HALO - k + STRIP]
                taps_acc[slot * count + k] += term[0:8] + term[8:16]
        return carry

    lax.fori_loop(0, seq // STRIP, unmix, 0)
    turn(((gg, gg_t), (gv, gv_t)))
    g_sent = first_stage(kinds[1], lambda cut: jnp.dot(gg_t[...], tok_all[cut], preferred_element_type=F32))
    v_sent = first_stage(kinds[2], lambda cut: jnp.dot(gv_t[...], tok_all[cut], preferred_element_type=F32))

    taps_mine[...] = jnp.sum(taps_acc[...], axis=1)
    taps_sent = []
    for offset in range(1, n):
        c = send(
            taps_mine, taps_in.at[me], t_send.at[offset - 1], t_recv.at[offset - 1],
            {"rep": lax.rem(me + offset, n)},
        )
        c.start()
        taps_sent.append(c)

    dn_passed = second_stage(kinds[0], dn_sent)
    ig_sent = []
    for slot, (spot, where) in enumerate(((far_spot, far), (diag_spot, diag), (core_spot, core), (mine, None))):
        rows = shard(spot)
        ig_part[rows, :] = (
            jnp.dot(gg[rows, :], gw[...], preferred_element_type=F32)
            + jnp.dot(gv[rows, :], vw[...], preferred_element_type=F32)
        ).astype(BF16)
        if where is not None:
            c = send(ig_part.at[rows, :], ig_in.at[slot], ig_send.at[slot], ig_recv.at[slot], where)
            c.start()
            ig_sent.append(c)
    dn_lines, dn_ends = third_stage(kinds[0], dn_passed)
    g_passed = second_stage(kinds[1], g_sent)
    dn_ends = fourth_stage(kinds[0], dn_lines, dn_ends)
    g_lines, g_ends = third_stage(kinds[1], g_passed)
    v_passed = second_stage(kinds[2], v_sent)
    g_ends = fourth_stage(kinds[1], g_lines, g_ends)
    v_lines, v_ends = third_stage(kinds[2], v_passed)

    for c in ig_sent:
        c.wait_recv()
    own = ig_part[shard(mine), :].astype(F32)
    for slot in range(3):
        own = own + ig_in[slot].astype(F32)
    ig_out[...] = own.astype(BF16)
    for c in taps_sent:
        c.wait_recv()
    taps_in[me] = taps_mine[...]
    total = taps_in[0]
    for slot in range(1, n):
        total = total + taps_in[slot]
    taps_out[...] = total * scale

    v_ends = fourth_stage(kinds[2], v_lines, v_ends)
    for c in dn_ends + g_ends + v_ends:
        c.wait_recv()
    for c in waits + taps_sent + ig_sent + [tok_far, tok_core, tok_relay, cot_far, cot_core, cot_relay]:
        c.wait_send()


def whole_layer(tokens, cotangent, gate_weight, value_weight, down_weight, gate_taps, value_taps, n, scale):
    depth = n // 2
    local, model = tokens.shape
    seq = 4 * local
    cols = gate_weight.shape[0]
    count = gate_taps.shape[0]
    dma = pltpu.SemaphoreType.DMA
    vmem = pl.BlockSpec(memory_space=pltpu.VMEM)
    cols_slots = pltpu.VMEM((depth, cols, model // n), BF16)
    return pl.pallas_call(
        functools.partial(layer_kernel, n, scale),
        out_shape=(
            jax.ShapeDtypeStruct((cols, model), BF16),
            jax.ShapeDtypeStruct((cols, model), BF16),
            jax.ShapeDtypeStruct((cols, model), BF16),
            jax.ShapeDtypeStruct((local, model), BF16),
            jax.ShapeDtypeStruct((2 * count, cols), F32),
        ),
        in_specs=[vmem] * 7,
        out_specs=(vmem,) * 5,
        scratch_shapes=[
            pltpu.VMEM((seq, model), BF16), pltpu.VMEM((seq, model), BF16),
            pltpu.VMEM((seq, cols), BF16), pltpu.VMEM((cols, seq), BF16),
            pltpu.VMEM((seq + HALO, cols), F32), pltpu.VMEM((seq + HALO, cols), F32),
            pltpu.VMEM((seq + HALO, cols), F32), pltpu.VMEM((seq + HALO, cols), F32),
            pltpu.VMEM((seq, cols), BF16), pltpu.VMEM((seq, cols), BF16),
            pltpu.VMEM((cols, seq), BF16), pltpu.VMEM((cols, seq), BF16),
            pltpu.VMEM((cols, model), BF16), pltpu.VMEM((cols, model), BF16), pltpu.VMEM((cols, model), BF16),
            pltpu.VMEM((seq, model), BF16),
            pltpu.VMEM((2 * count, 8, cols), F32), pltpu.VMEM((2 * count, cols), F32),
        ] + [cols_slots] * 9 + [
            pltpu.VMEM((3, local, model), BF16), pltpu.VMEM((n, 2 * count, cols), F32),
        ] + [dma((3,))] * 4 + [dma((3, depth))] * 8 + [dma((3,))] * 2 + [dma((n - 1,))] * 2,
        compiler_params=pltpu.CompilerParams(
            collective_id=0, has_side_effects=True, vmem_limit_bytes=60 * 1024 * 1024
        ),
    )(tokens, cotangent, gate_weight, value_weight, down_weight, gate_taps, value_taps)


def tiles_well(n, fs, tp, local, model, cols):
    return (
        n % 2 == 0 and fs == 2 and tp == 2 and model % (128 * n) == 0 and cols % 16 == 0 and local % 128 == 0
        and local * model <= 512 * 1024 and model * cols <= 1024 * 768
    )


def per_device(tokens, cotangent, gate_weight, value_weight, down_weight, gate_taps, value_taps):
    local_rows = tokens.shape[0]
    hidden_cols = gate_weight.shape[1]
    seq_len = local_rows * lax.axis_size("fs") * lax.axis_size("tp")
    total_tokens = seq_len * lax.axis_size("rep")
    scale = 1.0 / math.sqrt(total_tokens)
    n, fs, tp = lax.axis_size("rep"), lax.axis_size("fs"), lax.axis_size("tp")
    if tiles_well(n, fs, tp, local_rows, tokens.shape[1], hidden_cols):
        gate, value, down, input_grad, taps = whole_layer(
            tokens, cotangent, gate_weight.T, value_weight.T, down_weight, gate_taps, value_taps, n, scale
        )
        count = gate_taps.shape[0]
        return (
            input_grad, gate.astype(jnp.float32).T, value.astype(jnp.float32).T, down.astype(jnp.float32),
            taps[:count], taps[count:],
        )
    both_weights = jnp.concatenate([gate_weight, value_weight], axis=1)
    piece = lax.all_gather(tokens, ("fs", "tp"), axis=0, tiled=True)
    whole = piece
    block = jnp.dot(piece, both_weights, preferred_element_type=jnp.float32).astype(jnp.bfloat16)
    projected = block
    token_whole, projected = (whole, projected)
    piece = lax.all_gather(cotangent, ("fs", "tp"), axis=0, tiled=True)
    whole = piece
    back = contract_cols(piece, down_weight)
    up_gate = projected[:, :hidden_cols].astype(jnp.float32)
    up_value = projected[:, hidden_cols:].astype(jnp.float32)
    conv_gate = causal_mix(up_gate, gate_taps)
    conv_value = causal_mix(up_value, value_taps)
    sigma = jax.nn.sigmoid(conv_gate)
    silu_gate = conv_gate * sigma
    hidden = (silu_gate * conv_value).astype(jnp.bfloat16)
    back_value = back * silu_gate
    back_gate = back * conv_value * sigma * (1.0 + conv_gate * (1.0 - sigma))
    grad_gate = reverse_mix(back_gate, gate_taps).astype(jnp.bfloat16)
    grad_value = reverse_mix(back_value, value_taps).astype(jnp.bfloat16)
    tap_count = gate_taps.shape[0]
    input_grad = lax.psum_scatter(
        contract_cols(grad_gate, gate_weight) + contract_cols(grad_value, value_weight),
        ("fs", "tp"),
        scatter_dimension=0,
        tiled=True,
    ).astype(jnp.bfloat16)
    gate_part = contract_rows(token_whole, grad_gate)
    value_part = contract_rows(token_whole, grad_value)
    down_part = contract_rows(hidden, whole)
    gate_tap_part = tap_sums(back_gate, up_gate, tap_count)
    value_tap_part = tap_sums(back_value, up_value, tap_count)
    summed = lax.psum((gate_part, value_part, down_part, gate_tap_part, value_tap_part), "rep")
    weight_out = tuple((item * scale for item in summed))
    return (input_grad, weight_out[0], weight_out[1], weight_out[2], weight_out[3], weight_out[4])


def solution(mesh):
    in_specs = (
        P(("rep", "fs", "tp"), None),
        P(("rep", "fs", "tp"), None),
        P(None, ("fs", "tp")),
        P(None, ("fs", "tp")),
        P(("fs", "tp"), None),
        P(None, ("fs", "tp")),
        P(None, ("fs", "tp")),
    )
    out_specs = (
        P(("rep", "fs", "tp"), None),
        P(None, ("fs", "tp")),
        P(None, ("fs", "tp")),
        P(("fs", "tp"), None),
        P(None, ("fs", "tp")),
        P(None, ("fs", "tp")),
    )
    return jax.shard_map(
        per_device, mesh=mesh, in_specs=in_specs, out_specs=out_specs, check_vma=False
    )
```

```python
import functools
import math

import jax
import jax.numpy as jnp
from jax import lax
from jax.experimental import pallas as pl
from jax.experimental.pallas import tpu as pltpu
from jax.sharding import PartitionSpec as P


def shift_back(field, offset):
    return jnp.pad(field, ((offset, 0), (0, 0)))[: field.shape[0]]


def shift_ahead(field, offset):
    return jnp.pad(field, ((0, offset), (0, 0)))[offset:]


def causal_mix(field, taps):
    total = taps[0][None, :] * field
    for offset in range(1, taps.shape[0]):
        total = total + taps[offset][None, :] * shift_back(field, offset)
    return total


def reverse_mix(field, taps):
    total = taps[0][None, :] * field
    for offset in range(1, taps.shape[0]):
        total = total + taps[offset][None, :] * shift_ahead(field, offset)
    return total


def tap_sums(back, field, count):
    return jnp.stack([jnp.sum(back * shift_back(field, offset), axis=0) for offset in range(count)])


def contract_rows(left, right):
    return lax.dot_general(
        left, right, (((0,), (0,)), ((), ())), preferred_element_type=jnp.float32
    )


def contract_cols(left, right):
    return lax.dot_general(
        left, right, (((1,), (1,)), ((), ())), preferred_element_type=jnp.float32
    )

MESH = pl.DeviceIdType.MESH
BF16 = jnp.bfloat16
F32 = jnp.float32
STRIP = 16
HALO = 8


def send(src, dst, send_sem, recv_sem, where):
    return pltpu.make_async_remote_copy(
        src_ref=src, dst_ref=dst, send_sem=send_sem, recv_sem=recv_sem, device_id=where, device_id_type=MESH
    )


def layer_kernel(
    n, scale,
    tok, cot, gw, vw, dw, gt, vt,
    g_out, v_out, dn_out, ig_out, taps_out,
    tok_all, cot_all, hid, hid_t, up_g, up_v, bg, bv, gg, gv, gg_t, gv_t,
    g_part, v_part, dn_part, ig_part, taps_acc, taps_mine,
    g_y, v_y, dn_y, g_z, v_z, dn_z, g_in, v_in, dn_in, ig_in, taps_in,
    tok_send, tok_recv, cot_send, cot_recv,
    y_send, y_recv, z_send, z_recv, az_send, az_recv, ay_send, ay_recv, ig_send, ig_recv, t_send, t_recv,
):
    depth = n // 2
    me = lax.axis_index("rep")
    y, z = lax.rem(me, 2), lax.div(me, 2)
    partner = me + 1 - 2 * y
    my_fs, my_tp = lax.axis_index("fs"), lax.axis_index("tp")
    local = tok.shape[0]
    seq = 4 * local
    hidden_cols = gw.shape[0]
    count = gt.shape[0]
    mine = my_fs * 2 + my_tp
    core_spot = my_fs * 2 + 1 - my_tp
    far_spot = (1 - my_fs) * 2 + my_tp
    diag_spot = 3 - mine
    core, far, diag = {"tp": 1 - my_tp}, {"fs": 1 - my_fs}, {"fs": 1 - my_fs, "tp": 1 - my_tp}

    def shard(spot):
        return pl.ds(pl.multiple_of(spot * local, local), local)

    barrier = pltpu.get_barrier_semaphore()
    for offset in range(1, n):
        pl.semaphore_signal(barrier, inc=1, device_id={"rep": lax.rem(me + offset, n)}, device_id_type=MESH)
    for where in (core, far, diag):
        pl.semaphore_signal(barrier, inc=1, device_id=where, device_id_type=MESH)
    pl.semaphore_wait(barrier, n - 1 + 3)

    def gather(own, every, sends, recvs, slot, where):
        c = send(own, every.at[shard(mine), :], sends.at[slot], recvs.at[slot], where)
        c.start()
        return c

    def relay(every, sends, recvs):
        part = every.at[shard(far_spot), :]
        c = send(part, part, sends.at[2], recvs.at[2], core)
        c.start()
        return c

    tok_far = gather(tok, tok_all, tok_send, tok_recv, 0, far)
    tok_core = gather(tok, tok_all, tok_send, tok_recv, 1, core)
    cot_core = gather(cot, cot_all, cot_send, cot_recv, 1, core)
    tok_all[shard(mine), :] = tok[...]
    cot_all[shard(mine), :] = cot[...]
    zeros = jnp.zeros((HALO, hidden_cols), F32)
    up_g[0:HALO, :] = zeros
    up_v[0:HALO, :] = zeros
    bg[seq:seq + HALO, :] = zeros
    bv[seq:seq + HALO, :] = zeros
    taps_acc[...] = jnp.zeros_like(taps_acc)

    def project(spot):
        part = tok_all[shard(spot), :]
        rows = pl.ds(pl.multiple_of(spot * local + HALO, HALO), local)
        up_g[rows, :] = contract_cols(part, gw[...]).astype(BF16).astype(F32)
        up_v[rows, :] = contract_cols(part, vw[...]).astype(BF16).astype(F32)

    project(mine)
    tok_core.wait_recv()
    project(core_spot)
    tok_far.wait_recv()
    cot_far = gather(cot, cot_all, cot_send, cot_recv, 0, far)
    tok_relay = relay(tok_all, tok_send, tok_recv)
    project(far_spot)
    tok_relay.wait_recv()
    project(diag_spot)

    def mix(i, carry):
        start = pl.multiple_of(i * STRIP, STRIP)
        gs = up_g[pl.ds(start, STRIP + HALO), :]
        vs = up_v[pl.ds(start, STRIP + HALO), :]
        conv_gate = gt[0:1, :] * gs[HALO:HALO + STRIP]
        conv_value = vt[0:1, :] * vs[HALO:HALO + STRIP]
        for k in range(1, count):
            conv_gate = conv_gate + gt[k:k + 1, :] * gs[HALO - k:HALO - k + STRIP]
            conv_value = conv_value + vt[k:k + 1, :] * vs[HALO - k:HALO - k + STRIP]
        sigma = jax.nn.sigmoid(conv_gate)
        silu = conv_gate * sigma
        hid[pl.ds(start, STRIP), :] = (silu * conv_value).astype(BF16)
        bv[pl.ds(start, STRIP), :] = silu
        bg[pl.ds(start, STRIP), :] = conv_value * sigma * (1.0 + conv_gate * (1.0 - sigma))
        return carry

    lax.fori_loop(0, seq // STRIP, mix, 0)

    def turn(pairs):
        def step(i, carry):
            rows = pl.ds(pl.multiple_of(i * local, local), local)
            for flat, tall in pairs:
                tall[:, rows] = flat[rows, :].T
            return carry

        lax.fori_loop(0, 4, step, 0)

    turn(((hid, hid_t),))

    def pull_back(spot):
        rows = shard(spot)
        back = contract_cols(cot_all[rows, :], dw[...])
        bv[rows, :] = back * bv[rows, :]
        bg[rows, :] = back * bg[rows, :]

    pull_back(mine)
    cot_core.wait_recv()
    pull_back(core_spot)
    cot_far.wait_recv()
    cot_relay = relay(cot_all, cot_send, cot_recv)
    pull_back(far_spot)
    cot_relay.wait_recv()

    d_cols = dn_part.shape[1] // n

    def col_cut(chunk, width=1):
        return (slice(None), pl.ds(pl.multiple_of(chunk * d_cols, d_cols), d_cols * width))

    order = list(range(1, depth)) + [0]
    kinds = (
        (0, col_cut, dn_part, dn_y, dn_z, dn_in, dn_out),
        (1, col_cut, g_part, g_y, g_z, g_in, g_out),
        (2, col_cut, v_part, v_y, v_z, v_in, v_out),
    )
    waits = []

    def exchange(kind, k):
        index, cut, part, slots = kind[:4]
        theirs = 2 * lax.rem(z + k, depth) + 1 - y
        c = send(part.at[cut(theirs)], slots.at[k], y_send.at[index, k], y_recv.at[index, k], {"rep": partner})
        c.start()
        waits.append(c)
        return c

    def first_stage(kind, product):
        cut, part = kind[1], kind[2]
        sent = {}
        for k in order:
            pair = cut(2 * lax.rem(z + k, depth), 2)
            part[pair] = product(pair).astype(BF16)
            sent[k] = exchange(kind, k)
        return sent

    def second_stage(kind, sent):
        index, cut, part, slots, sums, arrivals = kind[:6]
        passed = []
        for k in order:
            ours = 2 * lax.rem(z + k, depth) + y
            sent[k].wait_recv()
            sums[k] = (part[cut(ours)].astype(F32) + slots[k].astype(F32)).astype(BF16)
            if k:
                c = send(sums.at[k], arrivals.at[k], z_send.at[index, k], z_recv.at[index, k], {"rep": ours})
                c.start()
                waits.append(c)
                passed.append(c)
        return passed

    def spread(kind, chunk, k, sends, recvs, where):
        index, cut, out = kind[0], kind[1], kind[6]
        c = send(out.at[cut(chunk)], out.at[cut(chunk)], sends.at[index, k], recvs.at[index, k], where)
        c.start()
        waits.append(c)
        return c

    def third_stage(kind, passed):
        cut, sums, arrivals, out = kind[1], kind[4], kind[5], kind[6]
        for c in passed:
            c.wait_recv()
        total = sums[0].astype(F32)
        for k in range(1, depth):
            total = total + arrivals[k].astype(F32)
        out[cut(me)] = (total * scale).astype(BF16)
        lines = [spread(kind, me, k, az_send, az_recv, {"rep": 2 * lax.rem(z + k, depth) + y}) for k in range(1, depth)]
        return lines, [spread(kind, me, 0, ay_send, ay_recv, {"rep": partner})]

    def fourth_stage(kind, lines, ends):
        for k in range(1, depth):
            lines[k - 1].wait_recv()
            chunk = 2 * lax.rem(z + depth - k, depth) + y
            ends.append(spread(kind, chunk, k, ay_send, ay_recv, {"rep": partner}))
        return ends

    pull_back(diag_spot)
    dn_sent = first_stage(
        kinds[0], lambda cut: jnp.dot(hid_t[...], cot_all[cut], preferred_element_type=F32)
    )

    def unmix(i, carry):
        start = pl.multiple_of(i * STRIP, STRIP)
        for slot, (field, back, taps, grad) in enumerate(((up_g, bg, gt, gg), (up_v, bv, vt, gv))):
            fs_ = field[pl.ds(start, STRIP + HALO), :]
            bs = back[pl.ds(start, STRIP + HALO), :]
            now = bs[0:STRIP]
            total = taps[0:1, :] * now
            for k in range(1, count):
                total = total + taps[k:k + 1, :] * bs[k:k + STRIP]
            grad[pl.ds(start, STRIP), :] = total.astype(BF16)
            for k in range(count):
                term = now * fs_[HALO - k:HALO - k + STRIP]
                taps_acc[slot * count + k] += term[0:8] + term[8:16]
        return carry

    lax.fori_loop(0, seq // STRIP, unmix, 0)
    turn(((gg, gg_t), (gv, gv_t)))
    g_sent = first_stage(kinds[1], lambda cut: jnp.dot(gg_t[...], tok_all[cut], preferred_element_type=F32))
    v_sent = first_stage(kinds[2], lambda cut: jnp.dot(gv_t[...], tok_all[cut], preferred_element_type=F32))

    taps_mine[...] = jnp.sum(taps_acc[...], axis=1)
    taps_sent = []
    for offset in range(1, n):
        c = send(
            taps_mine, taps_in.at[me], t_send.at[offset - 1], t_recv.at[offset - 1],
            {"rep": lax.rem(me + offset, n)},
        )
        c.start()
        taps_sent.append(c)

    dn_passed = second_stage(kinds[0], dn_sent)
    ig_sent = []
    for slot, (spot, where) in enumerate(((far_spot, far), (diag_spot, diag), (core_spot, core), (mine, None))):
        rows = shard(spot)
        ig_part[rows, :] = (
            jnp.dot(gg[rows, :], gw[...], preferred_element_type=F32)
            + jnp.dot(gv[rows, :], vw[...], preferred_element_type=F32)
        ).astype(BF16)
        if where is not None:
            c = send(ig_part.at[rows, :], ig_in.at[slot], ig_send.at[slot], ig_recv.at[slot], where)
            c.start()
            ig_sent.append(c)
    g_passed = second_stage(kinds[1], g_sent)
    dn_lines, dn_ends = third_stage(kinds[0], dn_passed)
    v_passed = second_stage(kinds[2], v_sent)
    g_lines, g_ends = third_stage(kinds[1], g_passed)
    dn_ends = fourth_stage(kinds[0], dn_lines, dn_ends)
    g_ends = fourth_stage(kinds[1], g_lines, g_ends)
    v_lines, v_ends = third_stage(kinds[2], v_passed)

    for c in ig_sent:
        c.wait_recv()
    own = ig_part[shard(mine), :].astype(F32)
    for slot in range(3):
        own = own + ig_in[slot].astype(F32)
    ig_out[...] = own.astype(BF16)
    for c in taps_sent:
        c.wait_recv()
    taps_in[me] = taps_mine[...]
    total = taps_in[0]
    for slot in range(1, n):
        total = total + taps_in[slot]
    taps_out[...] = total * scale

    v_ends = fourth_stage(kinds[2], v_lines, v_ends)
    for c in dn_ends + g_ends + v_ends:
        c.wait_recv()
    for c in waits + taps_sent + ig_sent + [tok_far, tok_core, tok_relay, cot_far, cot_core, cot_relay]:
        c.wait_send()


def whole_layer(tokens, cotangent, gate_weight, value_weight, down_weight, gate_taps, value_taps, n, scale):
    depth = n // 2
    local, model = tokens.shape
    seq = 4 * local
    cols = gate_weight.shape[0]
    count = gate_taps.shape[0]
    dma = pltpu.SemaphoreType.DMA
    vmem = pl.BlockSpec(memory_space=pltpu.VMEM)
    cols_slots = pltpu.VMEM((depth, cols, model // n), BF16)
    return pl.pallas_call(
        functools.partial(layer_kernel, n, scale),
        out_shape=(
            jax.ShapeDtypeStruct((cols, model), BF16),
            jax.ShapeDtypeStruct((cols, model), BF16),
            jax.ShapeDtypeStruct((cols, model), BF16),
            jax.ShapeDtypeStruct((local, model), BF16),
            jax.ShapeDtypeStruct((2 * count, cols), F32),
        ),
        in_specs=[vmem] * 7,
        out_specs=(vmem,) * 5,
        scratch_shapes=[
            pltpu.VMEM((seq, model), BF16), pltpu.VMEM((seq, model), BF16),
            pltpu.VMEM((seq, cols), BF16), pltpu.VMEM((cols, seq), BF16),
            pltpu.VMEM((seq + HALO, cols), F32), pltpu.VMEM((seq + HALO, cols), F32),
            pltpu.VMEM((seq + HALO, cols), F32), pltpu.VMEM((seq + HALO, cols), F32),
            pltpu.VMEM((seq, cols), BF16), pltpu.VMEM((seq, cols), BF16),
            pltpu.VMEM((cols, seq), BF16), pltpu.VMEM((cols, seq), BF16),
            pltpu.VMEM((cols, model), BF16), pltpu.VMEM((cols, model), BF16), pltpu.VMEM((cols, model), BF16),
            pltpu.VMEM((seq, model), BF16),
            pltpu.VMEM((2 * count, 8, cols), F32), pltpu.VMEM((2 * count, cols), F32),
        ] + [cols_slots] * 9 + [
            pltpu.VMEM((3, local, model), BF16), pltpu.VMEM((n, 2 * count, cols), F32),
        ] + [dma((3,))] * 4 + [dma((3, depth))] * 8 + [dma((3,))] * 2 + [dma((n - 1,))] * 2,
        compiler_params=pltpu.CompilerParams(
            collective_id=0, has_side_effects=True, vmem_limit_bytes=60 * 1024 * 1024
        ),
    )(tokens, cotangent, gate_weight, value_weight, down_weight, gate_taps, value_taps)


def tiles_well(n, fs, tp, local, model, cols):
    return (
        n % 2 == 0 and fs == 2 and tp == 2 and model % (128 * n) == 0 and cols % 16 == 0 and local % 128 == 0
        and local * model <= 512 * 1024 and model * cols <= 1024 * 768
    )


def per_device(tokens, cotangent, gate_weight, value_weight, down_weight, gate_taps, value_taps):
    local_rows = tokens.shape[0]
    hidden_cols = gate_weight.shape[1]
    seq_len = local_rows * lax.axis_size("fs") * lax.axis_size("tp")
    total_tokens = seq_len * lax.axis_size("rep")
    scale = 1.0 / math.sqrt(total_tokens)
    n, fs, tp = lax.axis_size("rep"), lax.axis_size("fs"), lax.axis_size("tp")
    if tiles_well(n, fs, tp, local_rows, tokens.shape[1], hidden_cols):
        gate, value, down, input_grad, taps = whole_layer(
            tokens, cotangent, gate_weight.T, value_weight.T, down_weight, gate_taps, value_taps, n, scale
        )
        count = gate_taps.shape[0]
        return (
            input_grad, gate.astype(jnp.float32).T, value.astype(jnp.float32).T, down.astype(jnp.float32),
            taps[:count], taps[count:],
        )
    both_weights = jnp.concatenate([gate_weight, value_weight], axis=1)
    piece = lax.all_gather(tokens, ("fs", "tp"), axis=0, tiled=True)
    whole = piece
    block = jnp.dot(piece, both_weights, preferred_element_type=jnp.float32).astype(jnp.bfloat16)
    projected = block
    token_whole, projected = (whole, projected)
    piece = lax.all_gather(cotangent, ("fs", "tp"), axis=0, tiled=True)
    whole = piece
    back = contract_cols(piece, down_weight)
    up_gate = projected[:, :hidden_cols].astype(jnp.float32)
    up_value = projected[:, hidden_cols:].astype(jnp.float32)
    conv_gate = causal_mix(up_gate, gate_taps)
    conv_value = causal_mix(up_value, value_taps)
    sigma = jax.nn.sigmoid(conv_gate)
    silu_gate = conv_gate * sigma
    hidden = (silu_gate * conv_value).astype(jnp.bfloat16)
    back_value = back * silu_gate
    back_gate = back * conv_value * sigma * (1.0 + conv_gate * (1.0 - sigma))
    grad_gate = reverse_mix(back_gate, gate_taps).astype(jnp.bfloat16)
    grad_value = reverse_mix(back_value, value_taps).astype(jnp.bfloat16)
    tap_count = gate_taps.shape[0]
    input_grad = lax.psum_scatter(
        contract_cols(grad_gate, gate_weight) + contract_cols(grad_value, value_weight),
        ("fs", "tp"),
        scatter_dimension=0,
        tiled=True,
    ).astype(jnp.bfloat16)
    gate_part = contract_rows(token_whole, grad_gate)
    value_part = contract_rows(token_whole, grad_value)
    down_part = contract_rows(hidden, whole)
    gate_tap_part = tap_sums(back_gate, up_gate, tap_count)
    value_tap_part = tap_sums(back_value, up_value, tap_count)
    summed = lax.psum((gate_part, value_part, down_part, gate_tap_part, value_tap_part), "rep")
    weight_out = tuple((item * scale for item in summed))
    return (input_grad, weight_out[0], weight_out[1], weight_out[2], weight_out[3], weight_out[4])


def solution(mesh):
    in_specs = (
        P(("rep", "fs", "tp"), None),
        P(("rep", "fs", "tp"), None),
        P(None, ("fs", "tp")),
        P(None, ("fs", "tp")),
        P(("fs", "tp"), None),
        P(None, ("fs", "tp")),
        P(None, ("fs", "tp")),
    )
    out_specs = (
        P(("rep", "fs", "tp"), None),
        P(None, ("fs", "tp")),
        P(None, ("fs", "tp")),
        P(("fs", "tp"), None),
        P(None, ("fs", "tp")),
        P(None, ("fs", "tp")),
    )
    return jax.shard_map(
        per_device, mesh=mesh, in_specs=in_specs, out_specs=out_specs, check_vma=False
    )
```
